32 devices in a mesh: gr: 2 (over core), sp: 8 (over z, y), tp: 2 (over x).
Axes of the slice: x: 2, y: 2, z: 4, core: 2. Of those that a mesh axis runs over, the one named last changes fastest.
Arguments:
- mixer_input: bfloat16 [16, 1536, 2048], P(('gr', 'tp'), 'sp'), may hold values from -16.8 to 16.8
- key_weight: bfloat16 [2048, 256], P('tp'), may hold values from -0.125 to 0.125
- content_projection_matrix: bfloat16 [2048, 256], P('tp'), may hold values from -0.125 to 0.125
- new_queries: bfloat16 [16, 32, 64], P(('gr', 'sp'), 'tp'), may hold values from -6 to 6
- head_stick_offset: float32 [32], replicated, may hold values from -11 to -4
Outputs:
- kv_cache: bfloat16 [16, 4, 1536, 128], P(('gr', 'sp'), 'tp')
- initial_attended_output: bfloat16 [16, 32, 64], P(('gr', 'sp'), 'tp')
The draws below stay inside these ranges and needn't reach their ends.
All inputs are finite; a program needn't handle non-finite values.
Results may differ from the reference program's by a relative error of at most 0.0081.
Values may be sent and summed in bfloat16 or wider, within the bound.
A program may use at most 64 MiB of HBM per device.

```python
import jax
import jax.numpy as jnp
from jax import lax

D = 2048
HEADS = 32
KV_HEADS = 4
HEAD_DIM = 64
BLOCK_POS = 192
CONTEXT_SPAN = 1536
BATCH_COUNT = 16
KV_SLOTS = 4


def draw_mixer_input(key, part):
    base_key = jax.random.fold_in(key, 11)
    scale_key = jax.random.fold_in(key, 12)
    arrival_draw_seed = jax.random.fold_in(key, 13)
    lookup_cells = jnp.clip(jax.random.normal(base_key, (BATCH_COUNT, CONTEXT_SPAN, D), jnp.float32), -4.0, 4.0)
    block_scale = jnp.exp(jax.random.uniform(scale_key, (BATCH_COUNT, CONTEXT_SPAN // BLOCK_POS, 1, 1), jnp.float32, jnp.log(0.35), jnp.log(1.4)))
    lookup_cells = (lookup_cells.reshape(BATCH_COUNT, CONTEXT_SPAN // BLOCK_POS, BLOCK_POS, D) * block_scale).reshape(BATCH_COUNT, CONTEXT_SPAN, D)
    arrival_clusters = jax.random.bernoulli(arrival_draw_seed, 4.0 / CONTEXT_SPAN, (BATCH_COUNT, CONTEXT_SPAN, 1))
    lookup_cells = lookup_cells * jnp.where(arrival_clusters, 3.0, 1.0)
    return lookup_cells.astype(jnp.bfloat16)


def draw_head_stick_offset(key, part):
    offset_key = jax.random.fold_in(key, 21)
    values_drawn = jax.random.uniform(offset_key, (HEADS,), jnp.float32, -9.5, -4.0)
    return values_drawn.astype(jnp.float32)


def levels(own_key, extent, pieces, smallest, high):
    def one(position, parts):
        steps = jax.random.uniform(jax.random.fold_in(jax.random.fold_in(own_key, 6), position), (parts,), jnp.float32, smallest / len(pieces), high / len(pieces))
        return jnp.repeat(jnp.exp(steps), extent[position] // parts).reshape((-1,) + (1,) * (len(extent) - position - 1))

    factor_of = one(*pieces[0])
    for cut in pieces[1:]:
        factor_of = factor_of * one(*cut)
    return factor_of


def centred(rng, dims, deviation, most, shards=(), held_as=jnp.bfloat16):
    array = deviation * jax.random.normal(rng, dims, jnp.float32)
    if shards:
        array = array * levels(rng, dims, shards, -0.22, 0.18)
    return jnp.clip(array, -most, most).astype(held_as)


def setup_inputs(seed: int = 0) -> dict:
    keys = jax.random.split(jax.random.key(seed), 6)
    mixer_input = draw_mixer_input(jax.random.fold_in(keys[5], 71), 0)
    key_weight = centred(keys[1], (D, KV_HEADS * HEAD_DIM), D ** -0.5, 0.125, ((0, 2),))
    content_projection_matrix = centred(keys[2], (D, KV_HEADS * HEAD_DIM), D ** -0.5, 0.125, ((0, 2),))
    new_queries = centred(keys[3], (BATCH_COUNT, HEADS, HEAD_DIM), 1.0, 6.0, ((0, 16), (1, 2)))
    head_stick_offset = draw_head_stick_offset(jax.random.fold_in(keys[5], 71), 0)
    return {"mixer_input": mixer_input, "key_weight": key_weight, "content_projection_matrix": content_projection_matrix, "new_queries": new_queries, "head_stick_offset": head_stick_offset}


def reference(mixer_input, key_weight, content_projection_matrix, new_queries, head_stick_offset):
    key_heads = key_weight.shape[1] // HEAD_DIM
    copies = KV_SLOTS // key_heads
    per_group = HEADS // key_heads
    offset_values = head_stick_offset.reshape(key_heads, per_group, 1)

    def one_sequence(operands):
        input_rows, query_rows = operands
        key_rows = jnp.dot(input_rows, key_weight, preferred_element_type=jnp.float32).astype(jnp.bfloat16)
        value_rows = jnp.dot(input_rows, content_projection_matrix, preferred_element_type=jnp.float32).astype(jnp.bfloat16)
        key_rows = key_rows.reshape(CONTEXT_SPAN, key_heads, HEAD_DIM).transpose(1, 0, 2)
        value_rows = value_rows.reshape(CONTEXT_SPAN, key_heads, HEAD_DIM).transpose(1, 0, 2)
        stacked = jnp.concatenate([key_rows, value_rows], axis=2)
        cache_rows = jnp.repeat(stacked, copies, axis=0)
        grouped = query_rows.reshape(key_heads, per_group, HEAD_DIM).astype(jnp.float32)
        logit_scores = jnp.einsum('hgd,hsd->hgs', grouped, key_rows.astype(jnp.float32)) * HEAD_DIM ** -0.5 + offset_values
        stay_terms = jax.nn.log_sigmoid(-logit_scores)
        later_terms = lax.cumsum(stay_terms, axis=2, reverse=True) - stay_terms
        weights = jnp.exp(jax.nn.log_sigmoid(logit_scores) + later_terms).astype(jnp.bfloat16)
        result = jnp.einsum('hgs,hsd->hgd', weights.astype(jnp.float32), value_rows.astype(jnp.float32))
        return cache_rows, result.reshape(HEADS, HEAD_DIM).astype(jnp.bfloat16)

    kv_cache, initial_attended_output = lax.map(one_sequence, (mixer_input, new_queries))
    return kv_cache, initial_attended_output
```

```python
import functools

import jax
import jax.numpy as jnp
from jax import lax
from jax.experimental import pallas as pl
from jax.experimental.pallas import tpu as pltpu
from jax.sharding import PartitionSpec as P

HEAD_DIM = 64
LANES = 128
MESH = pl.DeviceIdType.MESH


def kernel(
    sizes, x_hbm, k_hbm, v_hbm, q_ref, off_ref, cache_hbm, att_ref,
    x, w, acc, send, recv, x_sem, w_sem,
    s1, r1, s2, r2, s3, r3, s4, r4, out_sem,
):
    groups, spread, heads_dev, pair = sizes
    g, s, t = lax.axis_index("gr"), lax.axis_index("sp"), lax.axis_index("tp")
    seqs, block, width = x.shape
    rows = width // heads_dev
    piece = rows // (groups * pair)
    key_heads = send.shape[1]
    seq_local, slots, span = recv.shape[:3]
    copies = max(1, heads_dev // key_heads)
    side = lax.rem(s, pair)
    mate = s - side + lax.rem(side + 1, pair)

    w_loads = []
    for m, ref in enumerate((k_hbm, v_hbm)):
        load = pltpu.make_async_copy(
            ref, w.at[m, pl.ds(pl.multiple_of(t * rows, 8), rows)], w_sem.at[m]
        )
        load.start()
        w_loads.append(load)
    x_loads = []
    for i in range(seqs):
        load = pltpu.make_async_copy(x_hbm.at[i], x.at[i], x_sem.at[i])
        load.start()
        x_loads.append(load)

    barrier = pltpu.get_barrier_semaphore()
    members = spread * heads_dev
    me = s * heads_dev + t

    def greet(k, carry):
        other = lax.rem(me + k, members)
        pl.semaphore_signal(
            barrier, inc=1, device_id=(g, other // heads_dev, lax.rem(other, heads_dev)),
            device_id_type=MESH,
        )
        return carry

    lax.fori_loop(1, members, greet, 0)
    for k in range(1, groups):
        pl.semaphore_signal(
            barrier, inc=1, device_id=(lax.rem(g + k, groups), s, t), device_id_type=MESH
        )
    pl.semaphore_wait(barrier, members - 1 + groups - 1)

    def part(m, owner, group, half):
        start = pl.multiple_of(owner * rows + (group * pair + half) * piece, 8)
        return w.at[m, pl.ds(start, piece)]

    def remote(ref, send_sem, recv_sem, device):
        return pltpu.make_async_remote_copy(
            src_ref=ref, dst_ref=ref, send_sem=send_sem, recv_sem=recv_sem,
            device_id=device, device_id_type=MESH,
        )

    sent = []
    for m in range(2):
        w_loads[m].wait()
        for d in range(1, heads_dev):
            copy = remote(
                part(m, t, g, side), s1.at[m, d - 1], r1.at[m, d - 1],
                (g, s, lax.rem(t + d, heads_dev)),
            )
            copy.start()
            sent.append(copy)

    own = pl.ds(pl.multiple_of(t * rows, LANES), rows)
    half_cols = w.shape[2]

    def own_product(i):
        for m in range(2):
            acc[i, :, m * half_cols:(m + 1) * half_cols] = jnp.dot(
                x[i, :, own], w[m, own], preferred_element_type=jnp.float32
            )

    for i in range(seqs):
        x_loads[i].wait()
    own_product(0)

    for m in range(2):
        for d in range(1, heads_dev):
            owner = lax.rem(t + heads_dev - d, heads_dev)
            here = part(m, owner, g, side)
            remote(here, s1.at[m, d - 1], r1.at[m, d - 1], (g, s, t)).wait_recv()
            if pair > 1:
                copy = remote(here, s2.at[m, d - 1], r2.at[m, d - 1], (g, mate, t))
                copy.start()
                sent.append(copy)
            for k in range(1, groups):
                copy = remote(
                    here, s3.at[m, d - 1, 0, k - 1], r3.at[m, d - 1, 0, k - 1],
                    (lax.rem(g + k, groups), s, t),
                )
                copy.start()
                sent.append(copy)
        if m == 0:
            for i in range(1, seqs):
                own_product(i)
    if pair > 1:
        for m in range(2):
            for d in range(1, heads_dev):
                owner = lax.rem(t + heads_dev - d, heads_dev)
                there = part(m, owner, g, 1 - side)
                remote(there, s2.at[m, d - 1], r2.at[m, d - 1], (g, mate, t)).wait_recv()
                for k in range(1, groups):
                    copy = remote(
                        there, s3.at[m, d - 1, 1, k - 1], r3.at[m, d - 1, 1, k - 1],
                        (lax.rem(g + k, groups), s, t),
                    )
                    copy.start()
                    sent.append(copy)
    for m in range(2):
        for d in range(1, heads_dev):
            owner = lax.rem(t + heads_dev - d, heads_dev)
            for k in range(1, groups):
                source = lax.rem(g + groups - k, groups)
                for e in range(pair):
                    half = side if e == 0 else 1 - side
                    remote(
                        part(m, owner, source, half),
                        s3.at[m, d - 1, e, k - 1], r3.at[m, d - 1, e, k - 1],
                        (source, s, t),
                    ).wait_recv()

    def message(i, k):
        to = lax.rem(t + k, heads_dev)
        seq = t * seqs + i
        dst_s = seq // seq_local
        src = send.at[i, pl.ds(to * slots // copies, slots)]
        dst = recv.at[lax.rem(seq, seq_local), :, pl.ds(pl.multiple_of(s * block, 8), block)]
        return to, dst_s, src, dst, lax.rem(seq, seq_local)

    for i in range(seqs):
        total = []
        for m in range(2):
            value = acc[i, :, m * half_cols:(m + 1) * half_cols]
            for d in range(1, heads_dev):
                owner = lax.rem(t + d, heads_dev)
                cut = pl.ds(pl.multiple_of(owner * rows, LANES), rows)
                value = value + jnp.dot(
                    x[i, :, cut], w[m, cut], preferred_element_type=jnp.float32
                )
            total.append(value.astype(jnp.bfloat16))
        for h in range(key_heads):
            cut = slice(h * HEAD_DIM, (h + 1) * HEAD_DIM)
            send[i, h] = jnp.concatenate([total[0][:, cut], total[1][:, cut]], axis=1)
        for k in list(range(1, heads_dev)) + [0]:
            to, dst_s, src, dst, ql = message(i, k)
            local = jnp.logical_and(dst_s == s, to == t)

            @pl.when(local)
            def _():
                pltpu.make_async_copy(src, dst, r4.at[ql, s]).start()

            @pl.when(jnp.logical_not(local))
            def _():
                pltpu.make_async_remote_copy(
                    src_ref=src, dst_ref=dst, send_sem=s4.at[i, k], recv_sem=r4.at[ql, s],
                    device_id=(g, dst_s, to), device_id_type=MESH,
                ).start()

    for ql in range(seq_local):
        for b in range(spread):
            landed = recv.at[ql, :, pl.ds(b * block, block)]
            pltpu.make_async_copy(landed, landed, r4.at[ql, b]).wait()
            pltpu.make_async_copy(
                landed, cache_hbm.at[ql, :, pl.ds(b * block, block)], out_sem.at[ql, b]
            ).start()

    head_local = q_ref.shape[1]
    per_slot = head_local // slots
    row_id = lax.broadcasted_iota(jnp.int32, (per_slot, 1), 0)
    lane = lax.broadcasted_iota(jnp.int32, (per_slot, LANES), 1)
    for ql in range(seq_local):
        for u in range(slots):
            offset = jnp.zeros((per_slot, 1), jnp.float32)
            for j in range(per_slot):
                offset = jnp.where(
                    row_id == j, off_ref[t * head_local + u * per_slot + j], offset
                )
            q = q_ref[ql, u * per_slot:(u + 1) * per_slot, :]
            q = jnp.concatenate([q, jnp.zeros_like(q)], axis=1)
            later = jnp.zeros((per_slot, 1), jnp.float32)
            z = lax.dot_general(
                q, recv[ql, u], (((1,), (1,)), ((), ())), preferred_element_type=jnp.float32
            ) * HEAD_DIM ** -0.5 + offset
            stay = -(jnp.maximum(z, 0.0) + jnp.log1p(jnp.exp(-jnp.abs(z))))
            parts = []
            for c in range(span // LANES - 1, -1, -1):
                cols = slice(c * LANES, (c + 1) * LANES)
                run = stay[:, cols]
                step = 1
                while step < LANES:
                    moved = pltpu.roll(run, LANES - step, 1)
                    run = run + jnp.where(lane < LANES - step, moved, 0.0)
                    step *= 2
                parts.append(jnp.exp(z[:, cols] + (run + later)).astype(jnp.bfloat16))
                later = later + run[:, 0:1]
            weight = jnp.concatenate(parts[::-1], axis=1)
            result = jnp.dot(weight, recv[ql, u], preferred_element_type=jnp.float32)
            att_ref[ql, u * per_slot:(u + 1) * per_slot, :] = result[:, HEAD_DIM:].astype(
                jnp.bfloat16
            )

    for copy in sent:
        copy.wait_send()
    for i in range(seqs):
        for k in range(heads_dev):
            to, dst_s, src, dst, ql = message(i, k)

            @pl.when(jnp.logical_not(jnp.logical_and(dst_s == s, to == t)))
            def _():
                pltpu.make_async_remote_copy(
                    src_ref=src, dst_ref=dst, send_sem=s4.at[i, k], recv_sem=r4.at[ql, s],
                    device_id=(g, dst_s, to), device_id_type=MESH,
                ).wait_send()
    for ql in range(seq_local):
        for b in range(spread):
            landed = recv.at[ql, :, pl.ds(b * block, block)]
            pltpu.make_async_copy(
                landed, cache_hbm.at[ql, :, pl.ds(b * block, block)], out_sem.at[ql, b]
            ).wait()


def solution(mesh):
    groups, spread, heads_dev = mesh.shape["gr"], mesh.shape["sp"], mesh.shape["tp"]
    pair = 2 if spread % 2 == 0 else 1

    def local(mixer_input, key_weight, content_projection_matrix, new_queries, head_stick_offset):
        seqs, block, width = mixer_input.shape
        cols = key_weight.shape[1]
        key_heads = cols // HEAD_DIM
        seq_local, head_local = new_queries.shape[:2]
        slots = max(key_heads, heads_dev) // heads_dev
        span = block * spread
        others = heads_dev - 1
        dma = pltpu.SemaphoreType.DMA
        hbm = pl.BlockSpec(memory_space=pl.ANY)
        vmem = pl.BlockSpec(memory_space=pltpu.VMEM)
        return pl.pallas_call(
            functools.partial(kernel, (groups, spread, heads_dev, pair)),
            out_shape=(
                jax.ShapeDtypeStruct((seq_local, slots, span, 2 * HEAD_DIM), jnp.bfloat16),
                jax.ShapeDtypeStruct(new_queries.shape, jnp.bfloat16),
            ),
            in_specs=[hbm, hbm, hbm, vmem, pl.BlockSpec(memory_space=pltpu.SMEM)],
            out_specs=(hbm, vmem),
            scratch_shapes=[
                pltpu.VMEM((seqs, block, width), jnp.bfloat16),
                pltpu.VMEM((2, width, cols), jnp.bfloat16),
                pltpu.VMEM((seqs, block, 2 * cols), jnp.float32),
                pltpu.VMEM((seqs, key_heads, block, 2 * HEAD_DIM), jnp.bfloat16),
                pltpu.VMEM((seq_local, slots, span, 2 * HEAD_DIM), jnp.bfloat16),
                dma((seqs,)),
                dma((2,)),
                dma((2, others)),
                dma((2, others)),
                dma((2, others)),
                dma((2, others)),
                dma((2, others, 2, groups - 1)),
                dma((2, others, 2, groups - 1)),
                dma((seqs, heads_dev)),
                dma((seq_local, spread)),
                dma((seq_local, spread)),
            ],
            compiler_params=pltpu.CompilerParams(collective_id=0, has_side_effects=True),
        )(mixer_input, key_weight, content_projection_matrix, new_queries, head_stick_offset)

    return jax.shard_map(
        local,
        mesh=mesh,
        in_specs=(
            P(("gr", "tp"), "sp", None),
            P("tp", None),
            P("tp", None),
            P(("gr", "sp"), "tp", None),
            P(),
        ),
        out_specs=(P(("gr", "sp"), "tp", None, None), P(("gr", "sp"), "tp", None)),
        check_vma=False,
    )
```

```python
import functools

import jax
import jax.numpy as jnp
from jax import lax
from jax.experimental import pallas as pl
from jax.experimental.pallas import tpu as pltpu
from jax.sharding import PartitionSpec as P

HEAD_DIM = 64
LANES = 128
MESH = pl.DeviceIdType.MESH


def kernel(
    sizes, x_hbm, k_hbm, v_hbm, q_ref, off_ref, cache_hbm, att_ref,
    x, w, acc, send, stage, recv, x_sem, w_sem,
    s1, r1, s2, r2, s3, r3, s4, r4, s5, r5, out_sem,
):
    groups, spread, heads_dev, pair = sizes
    g, s, t = lax.axis_index("gr"), lax.axis_index("sp"), lax.axis_index("tp")
    seqs, block, width = x.shape
    rows = width // heads_dev
    piece = rows // (groups * pair)
    key_heads = send.shape[1]
    seq_local, slots, span = recv.shape[:3]
    copies = max(1, heads_dev // key_heads)
    side = lax.rem(s, pair)
    mate = s - side + lax.rem(side + 1, pair)

    w_loads = []
    for m, ref in enumerate((k_hbm, v_hbm)):
        load = pltpu.make_async_copy(
            ref, w.at[m, pl.ds(pl.multiple_of(t * rows, 8), rows)], w_sem.at[m]
        )
        load.start()
        w_loads.append(load)
    x_loads = []
    for i in range(seqs):
        load = pltpu.make_async_copy(x_hbm.at[i], x.at[i], x_sem.at[i])
        load.start()
        x_loads.append(load)

    barrier = pltpu.get_barrier_semaphore()
    members = spread * heads_dev
    me = s * heads_dev + t

    def greet(k, carry):
        other = lax.rem(me + k, members)
        pl.semaphore_signal(
            barrier, inc=1, device_id=(g, other // heads_dev, lax.rem(other, heads_dev)),
            device_id_type=MESH,
        )
        return carry

    lax.fori_loop(1, members, greet, 0)
    for k in range(1, groups):
        pl.semaphore_signal(
            barrier, inc=1, device_id=(lax.rem(g + k, groups), s, t), device_id_type=MESH
        )
    pl.semaphore_wait(barrier, members - 1 + groups - 1)

    def part(m, owner, group, half):
        start = pl.multiple_of(owner * rows + (group * pair + half) * piece, 8)
        return w.at[m, pl.ds(start, piece)]

    def remote(ref, send_sem, recv_sem, device):
        return pltpu.make_async_remote_copy(
            src_ref=ref, dst_ref=ref, send_sem=send_sem, recv_sem=recv_sem,
            device_id=device, device_id_type=MESH,
        )

    sent = []
    for m in range(2):
        w_loads[m].wait()
        for d in range(1, heads_dev):
            copy = remote(
                part(m, t, g, side), s1.at[m, d - 1], r1.at[m, d - 1],
                (g, s, lax.rem(t + d, heads_dev)),
            )
            copy.start()
            sent.append(copy)

    own = pl.ds(pl.multiple_of(t * rows, LANES), rows)
    half_cols = w.shape[2]

    def own_product(i):
        for m in range(2):
            acc[i, :, m * half_cols:(m + 1) * half_cols] = jnp.dot(
                x[i, :, own], w[m, own], preferred_element_type=jnp.float32
            )

    for i in range(seqs):
        x_loads[i].wait()
    own_product(0)

    for m in range(2):
        for d in range(1, heads_dev):
            owner = lax.rem(t + heads_dev - d, heads_dev)
            here = part(m, owner, g, side)
            remote(here, s1.at[m, d - 1], r1.at[m, d - 1], (g, s, t)).wait_recv()
            if pair > 1:
                copy = remote(here, s2.at[m, d - 1], r2.at[m, d - 1], (g, mate, t))
                copy.start()
                sent.append(copy)
            for k in range(1, groups):
                copy = remote(
                    here, s3.at[m, d - 1, 0, k - 1], r3.at[m, d - 1, 0, k - 1],
                    (lax.rem(g + k, groups), s, t),
                )
                copy.start()
                sent.append(copy)
        if m == 0:
            for i in range(1, seqs):
                own_product(i)
    if pair > 1:
        for m in range(2):
            for d in range(1, heads_dev):
                owner = lax.rem(t + heads_dev - d, heads_dev)
                there = part(m, owner, g, 1 - side)
                remote(there, s2.at[m, d - 1], r2.at[m, d - 1], (g, mate, t)).wait_recv()
                for k in range(1, groups):
                    copy = remote(
                        there, s3.at[m, d - 1, 1, k - 1], r3.at[m, d - 1, 1, k - 1],
                        (lax.rem(g + k, groups), s, t),
                    )
                    copy.start()
                    sent.append(copy)
    for m in range(2):
        for d in range(1, heads_dev):
            owner = lax.rem(t + heads_dev - d, heads_dev)
            for k in range(1, groups):
                source = lax.rem(g + groups - k, groups)
                for e in range(pair):
                    half = side if e == 0 else 1 - side
                    remote(
                        part(m, owner, source, half),
                        s3.at[m, d - 1, e, k - 1], r3.at[m, d - 1, e, k - 1],
                        (source, s, t),
                    ).wait_recv()

    def onward(k, i):
        seq = lax.rem(t + heads_dev - k, heads_dev) * seqs + i
        ql, dst_s = lax.rem(seq, seq_local), seq // seq_local
        src = send.at[i, pl.ds(t * slots // copies, slots)] if k == 0 else stage.at[k - 1, i]
        dst = recv.at[ql, :, pl.ds(pl.multiple_of(s * block, 8), block)]
        stays = dst_s == s
        inside = pltpu.make_async_copy(src, dst, r4.at[ql, s])
        outside = pltpu.make_async_remote_copy(
            src_ref=src, dst_ref=dst, send_sem=s4.at[k, i], recv_sem=r4.at[ql, s],
            device_id=(g, dst_s, t), device_id_type=MESH,
        )
        return stays, inside, outside

    def start_onward(k, i):
        stays, inside, outside = onward(k, i)
        pl.when(stays)(inside.start)
        pl.when(jnp.logical_not(stays))(outside.start)

    def across(k, i):
        to = lax.rem(t + k, heads_dev)
        return pltpu.make_async_remote_copy(
            src_ref=send.at[i, pl.ds(to * slots // copies, slots)], dst_ref=stage.at[k - 1, i],
            send_sem=s5.at[k - 1, i], recv_sem=r5.at[k - 1, i],
            device_id=(g, s, to), device_id_type=MESH,
        )

    for i in range(seqs):
        total = []
        for m in range(2):
            value = acc[i, :, m * half_cols:(m + 1) * half_cols]
            for d in range(1, heads_dev):
                owner = lax.rem(t + d, heads_dev)
                cut = pl.ds(pl.multiple_of(owner * rows, LANES), rows)
                value = value + jnp.dot(
                    x[i, :, cut], w[m, cut], preferred_element_type=jnp.float32
                )
            total.append(value.astype(jnp.bfloat16))
        for h in range(key_heads):
            cut = slice(h * HEAD_DIM, (h + 1) * HEAD_DIM)
            send[i, h] = jnp.concatenate([total[0][:, cut], total[1][:, cut]], axis=1)
        for k in range(1, heads_dev):
            across(k, i).start()
        start_onward(0, i)
    for i in range(seqs):
        for k in range(1, heads_dev):
            across(k, i).wait_recv()
            start_onward(k, i)

    for ql in range(seq_local):
        for b in range(spread):
            landed = recv.at[ql, :, pl.ds(b * block, block)]
            pltpu.make_async_copy(landed, landed, r4.at[ql, b]).wait()
            pltpu.make_async_copy(
                landed, cache_hbm.at[ql, :, pl.ds(b * block, block)], out_sem.at[ql, b]
            ).start()

    head_local = q_ref.shape[1]
    per_slot = head_local // slots
    row_id = lax.broadcasted_iota(jnp.int32, (per_slot, 1), 0)
    lane = lax.broadcasted_iota(jnp.int32, (per_slot, LANES), 1)
    for ql in range(seq_local):
        for u in range(slots):
            offset = jnp.zeros((per_slot, 1), jnp.float32)
            for j in range(per_slot):
                offset = jnp.where(
                    row_id == j, off_ref[t * head_local + u * per_slot + j], offset
                )
            q = q_ref[ql, u * per_slot:(u + 1) * per_slot, :]
            q = jnp.concatenate([q, jnp.zeros_like(q)], axis=1)
            later = jnp.zeros((per_slot, 1), jnp.float32)
            z = lax.dot_general(
                q, recv[ql, u], (((1,), (1,)), ((), ())), preferred_element_type=jnp.float32
            ) * HEAD_DIM ** -0.5 + offset
            stay = -(jnp.maximum(z, 0.0) + jnp.log1p(jnp.exp(-jnp.abs(z))))
            parts = []
            for c in range(span // LANES - 1, -1, -1):
                cols = slice(c * LANES, (c + 1) * LANES)
                run = stay[:, cols]
                step = 1
                while step < LANES:
                    moved = pltpu.roll(run, LANES - step, 1)
                    run = run + jnp.where(lane < LANES - step, moved, 0.0)
                    step *= 2
                parts.append(jnp.exp(z[:, cols] + (run + later)).astype(jnp.bfloat16))
                later = later + run[:, 0:1]
            weight = jnp.concatenate(parts[::-1], axis=1)
            result = jnp.dot(weight, recv[ql, u], preferred_element_type=jnp.float32)
            att_ref[ql, u * per_slot:(u + 1) * per_slot, :] = result[:, HEAD_DIM:].astype(
                jnp.bfloat16
            )

    for copy in sent:
        copy.wait_send()
    for i in range(seqs):
        for k in range(heads_dev):
            stays, inside, outside = onward(k, i)
            pl.when(jnp.logical_not(stays))(outside.wait_send)
            if k > 0:
                across(k, i).wait_send()
    for ql in range(seq_local):
        for b in range(spread):
            landed = recv.at[ql, :, pl.ds(b * block, block)]
            pltpu.make_async_copy(
                landed, cache_hbm.at[ql, :, pl.ds(b * block, block)], out_sem.at[ql, b]
            ).wait()


def solution(mesh):
    groups, spread, heads_dev = mesh.shape["gr"], mesh.shape["sp"], mesh.shape["tp"]
    pair = 2 if spread % 2 == 0 else 1

    def local(mixer_input, key_weight, content_projection_matrix, new_queries, head_stick_offset):
        seqs, block, width = mixer_input.shape
        cols = key_weight.shape[1]
        key_heads = cols // HEAD_DIM
        seq_local, head_local = new_queries.shape[:2]
        slots = max(key_heads, heads_dev) // heads_dev
        span = block * spread
        others = heads_dev - 1
        dma = pltpu.SemaphoreType.DMA
        hbm = pl.BlockSpec(memory_space=pl.ANY)
        vmem = pl.BlockSpec(memory_space=pltpu.VMEM)
        return pl.pallas_call(
            functools.partial(kernel, (groups, spread, heads_dev, pair)),
            out_shape=(
                jax.ShapeDtypeStruct((seq_local, slots, span, 2 * HEAD_DIM), jnp.bfloat16),
                jax.ShapeDtypeStruct(new_queries.shape, jnp.bfloat16),
            ),
            in_specs=[hbm, hbm, hbm, vmem, pl.BlockSpec(memory_space=pltpu.SMEM)],
            out_specs=(hbm, vmem),
            scratch_shapes=[
                pltpu.VMEM((seqs, block, width), jnp.bfloat16),
                pltpu.VMEM((2, width, cols), jnp.bfloat16),
                pltpu.VMEM((seqs, block, 2 * cols), jnp.float32),
                pltpu.VMEM((seqs, key_heads, block, 2 * HEAD_DIM), jnp.bfloat16),
                pltpu.VMEM((others, seqs, slots, block, 2 * HEAD_DIM), jnp.bfloat16),
                pltpu.VMEM((seq_local, slots, span, 2 * HEAD_DIM), jnp.bfloat16),
                dma((seqs,)),
                dma((2,)),
                dma((2, others)),
                dma((2, others)),
                dma((2, others)),
                dma((2, others)),
                dma((2, others, 2, groups - 1)),
                dma((2, others, 2, groups - 1)),
                dma((heads_dev, seqs)),
                dma((seq_local, spread)),
                dma((others, seqs)),
                dma((others, seqs)),
                dma((seq_local, spread)),
            ],
            compiler_params=pltpu.CompilerParams(collective_id=0, has_side_effects=True),
        )(mixer_input, key_weight, content_projection_matrix, new_queries, head_stick_offset)

    return jax.shard_map(
        local,
        mesh=mesh,
        in_specs=(
            P(("gr", "tp"), "sp", None),
            P("tp", None),
            P("tp", None),
            P(("gr", "sp"), "tp", None),
            P(),
        ),
        out_specs=(P(("gr", "sp"), "tp", None, None), P(("gr", "sp"), "tp", None)),
        check_vma=False,
    )
```

```python
import functools

import jax
import jax.numpy as jnp
from jax import lax
from jax.experimental import pallas as pl
from jax.experimental.pallas import tpu as pltpu
from jax.sharding import PartitionSpec as P

HEAD_DIM = 64
LANES = 128
CUTS = 2
MESH = pl.DeviceIdType.MESH


def kernel(
    sizes, x_hbm, k_hbm, v_hbm, q_ref, off_ref, cache_hbm, att_ref,
    x, w, acc, send, stage, recv, x_sem, w_sem,
    s1, r1, s2, r2, s3, r3, s4, r4, s5, r5, out_sem,
):
    groups, spread, heads_dev, pair = sizes
    g, s, t = lax.axis_index("gr"), lax.axis_index("sp"), lax.axis_index("tp")
    seqs, block, width = x.shape
    rows = width // heads_dev
    piece = rows // (groups * pair)
    key_heads = send.shape[1]
    seq_local, slots, span = recv.shape[:3]
    copies = max(1, heads_dev // key_heads)
    side = lax.rem(s, pair)
    mate = s - side + lax.rem(side + 1, pair)

    chunks, _, chunk_cols = w.shape
    wide = chunk_cols // 2
    chunk_heads = wide // HEAD_DIM

    def first(owner, e):
        return lax.rem((owner + 1) * slots // copies // chunk_heads + e, chunks)

    own_rows = pl.ds(pl.multiple_of(t * rows, LANES), rows)
    w_loads = []
    for c in range(chunks):
        for m, ref in enumerate((k_hbm, v_hbm)):
            load = pltpu.make_async_copy(
                ref.at[:, pl.ds(c * wide, wide)],
                w.at[c, own_rows, pl.ds(m * wide, wide)], w_sem.at[c, m],
            )
            load.start()
            w_loads.append(load)
    x_loads = []
    for i in range(seqs):
        load = pltpu.make_async_copy(x_hbm.at[i], x.at[i], x_sem.at[i])
        load.start()
        x_loads.append(load)

    barrier = pltpu.get_barrier_semaphore()
    members = spread * heads_dev
    me = s * heads_dev + t

    def greet(k, carry):
        other = lax.rem(me + k, members)
        pl.semaphore_signal(
            barrier, inc=1, device_id=(g, other // heads_dev, lax.rem(other, heads_dev)),
            device_id_type=MESH,
        )
        return carry

    lax.fori_loop(1, members, greet, 0)
    for k in range(1, groups):
        pl.semaphore_signal(
            barrier, inc=1, device_id=(lax.rem(g + k, groups), s, t), device_id_type=MESH
        )
    pl.semaphore_wait(barrier, members - 1 + groups - 1)

    def part(c, owner, group, half, f):
        start = owner * rows + (group * pair + half) * piece + f * (piece // CUTS)
        return w.at[c, pl.ds(pl.multiple_of(start, 8), piece // CUTS)]

    def remote(ref, send_sem, recv_sem, device):
        return pltpu.make_async_remote_copy(
            src_ref=ref, dst_ref=ref, send_sem=send_sem, recv_sem=recv_sem,
            device_id=device, device_id_type=MESH,
        )

    sent = []
    for load in w_loads:
        load.wait()
    for e in range(chunks):
        for f in range(CUTS):
            for d in range(1, heads_dev):
                to = lax.rem(t + d, heads_dev)
                copy = remote(
                    part(first(to, e), t, g, side, f), s1.at[e, f, d - 1], r1.at[e, f, d - 1],
                    (g, s, to),
                )
                copy.start()
                sent.append(copy)

    def owner_of(d):
        return lax.rem(t + heads_dev - d, heads_dev)

    def spread_piece(e, f, d, half, h):
        ref = part(first(t, e), owner_of(d), g, half, f)
        for k in range(1, groups):
            copy = remote(
                ref, s3.at[e, f, d - 1, h, k - 1], r3.at[e, f, d - 1, h, k - 1],
                (lax.rem(g + k, groups), s, t),
            )
            copy.start()
            sent.append(copy)

    def pass_first(e):
        for f in range(CUTS):
            for d in range(1, heads_dev):
                here = part(first(t, e), owner_of(d), g, side, f)
                remote(here, s1.at[e, f, d - 1], r1.at[e, f, d - 1], (g, s, t)).wait_recv()
                if pair > 1:
                    copy = remote(here, s2.at[e, f, d - 1], r2.at[e, f, d - 1], (g, mate, t))
                    copy.start()
                    sent.append(copy)
                spread_piece(e, f, d, side, 0)

    def pass_second(e):
        if pair > 1:
            for f in range(CUTS):
                for d in range(1, heads_dev):
                    there = part(first(t, e), owner_of(d), g, 1 - side, f)
                    remote(there, s2.at[e, f, d - 1], r2.at[e, f, d - 1], (g, mate, t)).wait_recv()
                    spread_piece(e, f, d, 1 - side, 1)

    def pass_last(e):
        for f in range(CUTS):
            for d in range(1, heads_dev):
                for k in range(1, groups):
                    source = lax.rem(g + groups - k, groups)
                    for h in range(pair):
                        remote(
                            part(first(t, e), owner_of(d), source, side if h == 0 else 1 - side, f),
                            s3.at[e, f, d - 1, h, k - 1], r3.at[e, f, d - 1, h, k - 1],
                            (source, s, t),
                        ).wait_recv()

    def own_product(e):
        for i in range(seqs):
            acc[e, i] = jnp.dot(
                x[i, :, own_rows], w[first(t, e), own_rows], preferred_element_type=jnp.float32
            )

    for i in range(seqs):
        x_loads[i].wait()
    for e in range(chunks):
        own_product(e)

    def onward(k, i):
        seq = lax.rem(t + heads_dev - k, heads_dev) * seqs + i
        ql, dst_s = lax.rem(seq, seq_local), seq // seq_local
        src = send.at[i, pl.ds(t * slots // copies, slots)] if k == 0 else stage.at[k - 1, i]
        dst = recv.at[ql, :, pl.ds(pl.multiple_of(s * block, 8), block)]
        stays = dst_s == s
        inside = pltpu.make_async_copy(src, dst, r4.at[ql, s])
        outside = pltpu.make_async_remote_copy(
            src_ref=src, dst_ref=dst, send_sem=s4.at[k, i], recv_sem=r4.at[ql, s],
            device_id=(g, dst_s, t), device_id_type=MESH,
        )
        return stays, inside, outside

    def start_onward(k, i):
        stays, inside, outside = onward(k, i)
        pl.when(stays)(inside.start)
        pl.when(jnp.logical_not(stays))(outside.start)

    def across(k, i):
        to = lax.rem(t + k, heads_dev)
        return pltpu.make_async_remote_copy(
            src_ref=send.at[i, pl.ds(to * slots // copies, slots)], dst_ref=stage.at[k - 1, i],
            send_sem=s5.at[k - 1, i], recv_sem=r5.at[k - 1, i],
            device_id=(g, s, to), device_id_type=MESH,
        )

    def finish(e):
        c = first(t, e)
        for i in range(seqs):
            value = acc[e, i]
            for d in range(1, heads_dev):
                cut = pl.ds(pl.multiple_of(lax.rem(t + d, heads_dev) * rows, LANES), rows)
                value = value + jnp.dot(
                    x[i, :, cut], w[c, cut], preferred_element_type=jnp.float32
                )
            value = value.astype(jnp.bfloat16)
            for h in range(chunk_heads):
                low = h * HEAD_DIM
                send[i, c * chunk_heads + h] = jnp.concatenate(
                    [value[:, low:low + HEAD_DIM], value[:, wide + low:wide + low + HEAD_DIM]],
                    axis=1,
                )
            for k in list(range(1, heads_dev)) + [0]:
                to = lax.rem(t + k, heads_dev)

                @pl.when(to * slots // copies // chunk_heads == c)
                def _():
                    if k:
                        across(k, i).start()
                    else:
                        start_onward(0, i)

    for e in range(chunks):
        pass_first(e)
    for e in range(chunks):
        pass_second(e)
        pass_last(e)
        finish(e)
    for i in range(seqs):
        for k in range(1, heads_dev):
            across(k, i).wait_recv()
            start_onward(k, i)

    for ql in range(seq_local):
        for b in range(spread):
            landed = recv.at[ql, :, pl.ds(b * block, block)]
            pltpu.make_async_copy(landed, landed, r4.at[ql, b]).wait()
            pltpu.make_async_copy(
                landed, cache_hbm.at[ql, :, pl.ds(b * block, block)], out_sem.at[ql, b]
            ).start()

    head_local = q_ref.shape[1]
    per_slot = head_local // slots
    row_id = lax.broadcasted_iota(jnp.int32, (per_slot, 1), 0)
    lane = lax.broadcasted_iota(jnp.int32, (per_slot, LANES), 1)
    for ql in range(seq_local):
        for u in range(slots):
            offset = jnp.zeros((per_slot, 1), jnp.float32)
            for j in range(per_slot):
                offset = jnp.where(
                    row_id == j, off_ref[t * head_local + u * per_slot + j], offset
                )
            q = q_ref[ql, u * per_slot:(u + 1) * per_slot, :]
            q = jnp.concatenate([q, jnp.zeros_like(q)], axis=1)
            later = jnp.zeros((per_slot, 1), jnp.float32)
            z = lax.dot_general(
                q, recv[ql, u], (((1,), (1,)), ((), ())), preferred_element_type=jnp.float32
            ) * HEAD_DIM ** -0.5 + offset
            stay = -(jnp.maximum(z, 0.0) + jnp.log1p(jnp.exp(-jnp.abs(z))))
            parts = []
            for c in range(span // LANES - 1, -1, -1):
                cols = slice(c * LANES, (c + 1) * LANES)
                run = stay[:, cols]
                step = 1
                while step < LANES:
                    moved = pltpu.roll(run, LANES - step, 1)
                    run = run + jnp.where(lane < LANES - step, moved, 0.0)
                    step *= 2
                parts.append(jnp.exp(z[:, cols] + (run + later)).astype(jnp.bfloat16))
                later = later + run[:, 0:1]
            weight = jnp.concatenate(parts[::-1], axis=1)
            result = jnp.dot(weight, recv[ql, u], preferred_element_type=jnp.float32)
            att_ref[ql, u * per_slot:(u + 1) * per_slot, :] = result[:, HEAD_DIM:].astype(
                jnp.bfloat16
            )

    for copy in sent:
        copy.wait_send()
    for i in range(seqs):
        for k in range(heads_dev):
            stays, inside, outside = onward(k, i)
            pl.when(jnp.logical_not(stays))(outside.wait_send)
            if k > 0:
                across(k, i).wait_send()
    for ql in range(seq_local):
        for b in range(spread):
            landed = recv.at[ql, :, pl.ds(b * block, block)]
            pltpu.make_async_copy(
                landed, cache_hbm.at[ql, :, pl.ds(b * block, block)], out_sem.at[ql, b]
            ).wait()


def solution(mesh):
    groups, spread, heads_dev = mesh.shape["gr"], mesh.shape["sp"], mesh.shape["tp"]
    pair = 2 if spread % 2 == 0 else 1

    def local(mixer_input, key_weight, content_projection_matrix, new_queries, head_stick_offset):
        seqs, block, width = mixer_input.shape
        cols = key_weight.shape[1]
        key_heads = cols // HEAD_DIM
        seq_local, head_local = new_queries.shape[:2]
        slots = max(key_heads, heads_dev) // heads_dev
        span = block * spread
        others = heads_dev - 1
        wide = max(LANES, slots * HEAD_DIM)
        chunks = cols // wide
        dma = pltpu.SemaphoreType.DMA
        hbm = pl.BlockSpec(memory_space=pl.ANY)
        vmem = pl.BlockSpec(memory_space=pltpu.VMEM)
        return pl.pallas_call(
            functools.partial(kernel, (groups, spread, heads_dev, pair)),
            out_shape=(
                jax.ShapeDtypeStruct((seq_local, slots, span, 2 * HEAD_DIM), jnp.bfloat16),
                jax.ShapeDtypeStruct(new_queries.shape, jnp.bfloat16),
            ),
            in_specs=[hbm, hbm, hbm, vmem, pl.BlockSpec(memory_space=pltpu.SMEM)],
            out_specs=(hbm, vmem),
            scratch_shapes=[
                pltpu.VMEM((seqs, block, width), jnp.bfloat16),
                pltpu.VMEM((chunks, width, 2 * wide), jnp.bfloat16),
                pltpu.VMEM((chunks, seqs, block, 2 * wide), jnp.float32),
                pltpu.VMEM((seqs, key_heads, block, 2 * HEAD_DIM), jnp.bfloat16),
                pltpu.VMEM((others, seqs, slots, block, 2 * HEAD_DIM), jnp.bfloat16),
                pltpu.VMEM((seq_local, slots, span, 2 * HEAD_DIM), jnp.bfloat16),
                dma((seqs,)),
                dma((chunks, 2)),
                dma((chunks, CUTS, others)),
                dma((chunks, CUTS, others)),
                dma((chunks, CUTS, others)),
                dma((chunks, CUTS, others)),
                dma((chunks, CUTS, others, 2, groups - 1)),
                dma((chunks, CUTS, others, 2, groups - 1)),
                dma((heads_dev, seqs)),
                dma((seq_local, spread)),
                dma((others, seqs)),
                dma((others, seqs)),
                dma((seq_local, spread)),
            ],
            compiler_params=pltpu.CompilerParams(collective_id=0, has_side_effects=True),
        )(mixer_input, key_weight, content_projection_matrix, new_queries, head_stick_offset)

    return jax.shard_map(
        local,
        mesh=mesh,
        in_specs=(
            P(("gr", "tp"), "sp", None),
            P("tp", None),
            P("tp", None),
            P(("gr", "sp"), "tp", None),
            P(),
        ),
        out_specs=(P(("gr", "sp"), "tp", None, None), P(("gr", "sp"), "tp", None)),
        check_vma=False,
    )
```

```python
import functools

import jax
import jax.numpy as jnp
from jax import lax
from jax.experimental import pallas as pl
from jax.experimental.pallas import tpu as pltpu
from jax.sharding import PartitionSpec as P

HEAD_DIM = 64
LANES = 128
CUTS = 2
MESH = pl.DeviceIdType.MESH


def kernel(
    sizes, x_hbm, k_hbm, v_hbm, recv,
    x, w, acc, send, stage, x_sem, w_sem,
    s1, r1, s2, r2, s3, r3, s4, r4, s5, r5,
):
    groups, spread, heads_dev, pair = sizes
    g, s, t = lax.axis_index("gr"), lax.axis_index("sp"), lax.axis_index("tp")
    seqs, block, width = x.shape
    rows = width // heads_dev
    piece = rows // (groups * pair)
    key_heads = send.shape[1]
    seq_local, slots, span = recv.shape[:3]
    copies = max(1, heads_dev // key_heads)
    side = lax.rem(s, pair)
    mate = s - side + lax.rem(side + 1, pair)

    chunks, _, chunk_cols = w.shape
    wide = chunk_cols // 2
    chunk_heads = wide // HEAD_DIM

    def first(owner, e):
        return lax.rem((owner + 1) * slots // copies // chunk_heads + e, chunks)

    own_rows = pl.ds(pl.multiple_of(t * rows, LANES), rows)
    w_loads = []
    for c in range(chunks):
        for m, ref in enumerate((k_hbm, v_hbm)):
            load = pltpu.make_async_copy(
                ref.at[:, pl.ds(c * wide, wide)],
                w.at[c, own_rows, pl.ds(m * wide, wide)], w_sem.at[c, m],
            )
            load.start()
            w_loads.append(load)
    x_loads = []
    for i in range(seqs):
        load = pltpu.make_async_copy(x_hbm.at[i], x.at[i], x_sem.at[i])
        load.start()
        x_loads.append(load)

    barrier = pltpu.get_barrier_semaphore()
    members = spread * heads_dev
    me = s * heads_dev + t

    def greet(k, carry):
        other = lax.rem(me + k, members)
        pl.semaphore_signal(
            barrier, inc=1, device_id=(g, other // heads_dev, lax.rem(other, heads_dev)),
            device_id_type=MESH,
        )
        return carry

    lax.fori_loop(1, members, greet, 0)
    for k in range(1, groups):
        pl.semaphore_signal(
            barrier, inc=1, device_id=(lax.rem(g + k, groups), s, t), device_id_type=MESH
        )
    pl.semaphore_wait(barrier, members - 1 + groups - 1)

    def part(c, owner, group, half, f):
        start = owner * rows + (group * pair + half) * piece + f * (piece // CUTS)
        return w.at[c, pl.ds(pl.multiple_of(start, 8), piece // CUTS)]

    def remote(ref, send_sem, recv_sem, device):
        return pltpu.make_async_remote_copy(
            src_ref=ref, dst_ref=ref, send_sem=send_sem, recv_sem=recv_sem,
            device_id=device, device_id_type=MESH,
        )

    sent = []
    for load in w_loads:
        load.wait()
    for e in range(chunks):
        for f in range(CUTS):
            for d in range(1, heads_dev):
                to = lax.rem(t + d, heads_dev)
                copy = remote(
                    part(first(to, e), t, g, side, f), s1.at[e, f, d - 1], r1.at[e, f, d - 1],
                    (g, s, to),
                )
                copy.start()
                sent.append(copy)

    def owner_of(d):
        return lax.rem(t + heads_dev - d, heads_dev)

    def spread_piece(e, f, d, half, h):
        ref = part(first(t, e), owner_of(d), g, half, f)
        for k in range(1, groups):
            copy = remote(
                ref, s3.at[e, f, d - 1, h, k - 1], r3.at[e, f, d - 1, h, k - 1],
                (lax.rem(g + k, groups), s, t),
            )
            copy.start()
            sent.append(copy)

    def pass_first(e):
        for f in range(CUTS):
            for d in range(1, heads_dev):
                here = part(first(t, e), owner_of(d), g, side, f)
                remote(here, s1.at[e, f, d - 1], r1.at[e, f, d - 1], (g, s, t)).wait_recv()
                if pair > 1:
                    copy = remote(here, s2.at[e, f, d - 1], r2.at[e, f, d - 1], (g, mate, t))
                    copy.start()
                    sent.append(copy)
                spread_piece(e, f, d, side, 0)

    def pass_second(e):
        if pair > 1:
            for f in range(CUTS):
                for d in range(1, heads_dev):
                    there = part(first(t, e), owner_of(d), g, 1 - side, f)
                    remote(there, s2.at[e, f, d - 1], r2.at[e, f, d - 1], (g, mate, t)).wait_recv()
                    spread_piece(e, f, d, 1 - side, 1)

    def pass_last(e):
        for f in range(CUTS):
            for d in range(1, heads_dev):
                for k in range(1, groups):
                    source = lax.rem(g + groups - k, groups)
                    for h in range(pair):
                        remote(
                            part(first(t, e), owner_of(d), source, side if h == 0 else 1 - side, f),
                            s3.at[e, f, d - 1, h, k - 1], r3.at[e, f, d - 1, h, k - 1],
                            (source, s, t),
                        ).wait_recv()

    def own_product(e):
        for i in range(seqs):
            acc[e, i] = jnp.dot(
                x[i, :, own_rows], w[first(t, e), own_rows], preferred_element_type=jnp.float32
            )

    for i in range(seqs):
        x_loads[i].wait()
    for e in range(chunks):
        own_product(e)

    def onward(k, i):
        seq = lax.rem(t + heads_dev - k, heads_dev) * seqs + i
        ql, dst_s = lax.rem(seq, seq_local), seq // seq_local
        src = send.at[i, pl.ds(t * slots // copies, slots)] if k == 0 else stage.at[k - 1, i]
        dst = recv.at[ql, :, pl.ds(pl.multiple_of(s * block, 8), block)]
        stays = dst_s == s
        inside = pltpu.make_async_copy(src, dst, r4.at[ql, s])
        outside = pltpu.make_async_remote_copy(
            src_ref=src, dst_ref=dst, send_sem=s4.at[k, i], recv_sem=r4.at[ql, s],
            device_id=(g, dst_s, t), device_id_type=MESH,
        )
        return stays, inside, outside

    def start_onward(k, i):
        stays, inside, outside = onward(k, i)
        pl.when(stays)(inside.start)
        pl.when(jnp.logical_not(stays))(outside.start)

    def across(k, i):
        to = lax.rem(t + k, heads_dev)
        return pltpu.make_async_remote_copy(
            src_ref=send.at[i, pl.ds(to * slots // copies, slots)], dst_ref=stage.at[k - 1, i],
            send_sem=s5.at[k - 1, i], recv_sem=r5.at[k - 1, i],
            device_id=(g, s, to), device_id_type=MESH,
        )

    def finish(e, i):
        c = first(t, e)
        value = acc[e, i]
        for d in range(1, heads_dev):
            cut = pl.ds(pl.multiple_of(lax.rem(t + d, heads_dev) * rows, LANES), rows)
            value = value + jnp.dot(
                x[i, :, cut], w[c, cut], preferred_element_type=jnp.float32
            )
        value = value.astype(jnp.bfloat16)
        for h in range(chunk_heads):
            low = h * HEAD_DIM
            send[i, c * chunk_heads + h] = jnp.concatenate(
                [value[:, low:low + HEAD_DIM], value[:, wide + low:wide + low + HEAD_DIM]],
                axis=1,
            )
        for k in list(range(1, heads_dev)) + [0]:
            to = lax.rem(t + k, heads_dev)

            @pl.when(to * slots // copies // chunk_heads == c)
            def _():
                if k:
                    across(k, i).start()
                else:
                    start_onward(0, i)

    for e in range(chunks):
        pass_first(e)
    for e in range(chunks):
        pass_second(e)
        pass_last(e)
        for i in range(seqs):
            finish(e, i)
            if e == chunks - 1:
                for k in range(1, heads_dev):
                    across(k, i).wait_recv()
                    start_onward(k, i)

    for ql in range(seq_local):
        for b in range(spread):
            landed = recv.at[ql, :, pl.ds(b * block, block)]
            pltpu.make_async_copy(landed, landed, r4.at[ql, b]).wait()

    for copy in sent:
        copy.wait_send()
    for i in range(seqs):
        for k in range(heads_dev):
            stays, inside, outside = onward(k, i)
            pl.when(jnp.logical_not(stays))(outside.wait_send)
            if k > 0:
                across(k, i).wait_send()

def read_kernel(recv, q_ref, off_ref, cache_hbm, att_ref, out_sem):
    t = lax.axis_index("tp")
    seq_local, slots, span = recv.shape[:3]
    keep = pltpu.make_async_copy(recv, cache_hbm, out_sem)
    keep.start()

    head_local = q_ref.shape[1]
    per_slot = head_local // slots
    row_id = lax.broadcasted_iota(jnp.int32, (per_slot, 1), 0)
    lane = lax.broadcasted_iota(jnp.int32, (per_slot, LANES), 1)
    for ql in range(seq_local):
        for u in range(slots):
            offset = jnp.zeros((per_slot, 1), jnp.float32)
            for j in range(per_slot):
                offset = jnp.where(
                    row_id == j, off_ref[t * head_local + u * per_slot + j], offset
                )
            q = q_ref[ql, u * per_slot:(u + 1) * per_slot, :]
            q = jnp.concatenate([q, jnp.zeros_like(q)], axis=1)
            later = jnp.zeros((per_slot, 1), jnp.float32)
            z = lax.dot_general(
                q, recv[ql, u], (((1,), (1,)), ((), ())), preferred_element_type=jnp.float32
            ) * HEAD_DIM ** -0.5 + offset
            stay = -(jnp.maximum(z, 0.0) + jnp.log1p(jnp.exp(-jnp.abs(z))))
            parts = []
            for c in range(span // LANES - 1, -1, -1):
                cols = slice(c * LANES, (c + 1) * LANES)
                run = stay[:, cols]
                step = 1
                while step < LANES:
                    moved = pltpu.roll(run, LANES - step, 1)
                    run = run + jnp.where(lane < LANES - step, moved, 0.0)
                    step *= 2
                parts.append(jnp.exp(z[:, cols] + (run + later)).astype(jnp.bfloat16))
                later = later + run[:, 0:1]
            weight = jnp.concatenate(parts[::-1], axis=1)
            result = jnp.dot(weight, recv[ql, u], preferred_element_type=jnp.float32)
            att_ref[ql, u * per_slot:(u + 1) * per_slot, :] = result[:, HEAD_DIM:].astype(
                jnp.bfloat16
            )

    keep.wait()


def solution(mesh):
    groups, spread, heads_dev = mesh.shape["gr"], mesh.shape["sp"], mesh.shape["tp"]
    pair = 2 if spread % 2 == 0 else 1

    def local(mixer_input, key_weight, content_projection_matrix, new_queries, head_stick_offset):
        seqs, block, width = mixer_input.shape
        cols = key_weight.shape[1]
        key_heads = cols // HEAD_DIM
        seq_local, head_local = new_queries.shape[:2]
        slots = max(key_heads, heads_dev) // heads_dev
        span = block * spread
        others = heads_dev - 1
        wide = max(LANES, slots * HEAD_DIM)
        chunks = cols // wide
        dma = pltpu.SemaphoreType.DMA
        hbm = pl.BlockSpec(memory_space=pl.ANY)
        vmem = pl.BlockSpec(memory_space=pltpu.VMEM)
        cache_shape = (seq_local, slots, span, 2 * HEAD_DIM)
        landed = pl.pallas_call(
            functools.partial(kernel, (groups, spread, heads_dev, pair)),
            out_shape=pltpu.VMEM(cache_shape, jnp.bfloat16),
            in_specs=[hbm, hbm, hbm],
            out_specs=vmem,
            scratch_shapes=[
                pltpu.VMEM((seqs, block, width), jnp.bfloat16),
                pltpu.VMEM((chunks, width, 2 * wide), jnp.bfloat16),
                pltpu.VMEM((chunks, seqs, block, 2 * wide), jnp.float32),
                pltpu.VMEM((seqs, key_heads, block, 2 * HEAD_DIM), jnp.bfloat16),
                pltpu.VMEM((others, seqs, slots, block, 2 * HEAD_DIM), jnp.bfloat16),
                dma((seqs,)),
                dma((chunks, 2)),
                dma((chunks, CUTS, others)),
                dma((chunks, CUTS, others)),
                dma((chunks, CUTS, others)),
                dma((chunks, CUTS, others)),
                dma((chunks, CUTS, others, 2, groups - 1)),
                dma((chunks, CUTS, others, 2, groups - 1)),
                dma((heads_dev, seqs)),
                dma((seq_local, spread)),
                dma((others, seqs)),
                dma((others, seqs)),
            ],
            compiler_params=pltpu.CompilerParams(
                collective_id=0, has_side_effects=True
            ),
        )(mixer_input, key_weight, content_projection_matrix)
        return pl.pallas_call(
            read_kernel,
            out_shape=(
                jax.ShapeDtypeStruct(cache_shape, jnp.bfloat16),
                jax.ShapeDtypeStruct(new_queries.shape, jnp.bfloat16),
            ),
            in_specs=[vmem, vmem, pl.BlockSpec(memory_space=pltpu.SMEM)],
            out_specs=(hbm, vmem),
            scratch_shapes=[pltpu.SemaphoreType.DMA],
            compiler_params=pltpu.CompilerParams(vmem_limit_bytes=16 * 2**20),
        )(landed, new_queries, head_stick_offset)

    return jax.shard_map(
        local,
        mesh=mesh,
        in_specs=(
            P(("gr", "tp"), "sp", None),
            P("tp", None),
            P("tp", None),
            P(("gr", "sp"), "tp", None),
            P(),
        ),
        out_specs=(P(("gr", "sp"), "tp", None, None), P(("gr", "sp"), "tp", None)),
        check_vma=False,
    )
```
